32 devices in a mesh: sp: 16 (over z, y, x), tp: 2 (over core).
Axes of the slice: x: 2, y: 2, z: 4, core: 2. Of those that a mesh axis runs over, the one named last changes fastest.
Arguments:
- tokens: bfloat16 [1024, 1, 2048], P('sp'), may hold values from -6 to 6
- queries: bfloat16 [1024, 1, 1024], P('sp', None, 'tp'), may hold values from -15 to 15
- key_values: bfloat16 [1024, 1, 1024], P('sp', None, 'tp'), may hold values from -6 to 6
- stop_bias: bfloat16 [1024, 1, 16], P('sp', None, 'tp'), may hold values from -20 to 0
- out_proj: bfloat16 [1024, 2048], P('tp'), may hold values from -0.375 to 0.375
- norm_gain: float32 [2048], replicated, may hold values from 0.1 to 1.9
- up_proj: bfloat16 [2048, 4096], P('sp', 'tp'), may hold values from -0.125 to 0.125
- down_proj: bfloat16 [4096, 2048], P('tp', 'sp'), may hold values from -0.09375 to 0.09375
Outputs:
- layer_out: bfloat16 [1024, 1, 2048], P(('sp', 'tp'))
The draws below stay inside these ranges and needn't reach their ends.
All inputs are finite; a program needn't handle non-finite values.
Results may differ from the reference program's by a relative error of at most 0.018.
Values may be sent and summed in bfloat16 or wider, within the bound.
A program may use at most 64 MiB of HBM per device.

```python
import jax
import jax.numpy as jnp
from jax import lax

D = 2048
FF = 4096
QUERY_HEAD_COUNT = 16
KV_HEADS = 8
HEAD = 64
SEQUENCE_COUNT = 1
TOK_DEV = 64
TOKEN_LENGTH = 1024
N_TP = 2


def draw_stop_bias(key, part):
    key_tensor = jax.random.split(key, 7)
    fast_heads = jax.random.randint(key_tensor[0], (SEQUENCE_COUNT, QUERY_HEAD_COUNT), 0, 2) == 0
    slow_level = -jnp.log(jnp.float32(TOKEN_LENGTH)) - jax.random.uniform(key_tensor[1], (SEQUENCE_COUNT, QUERY_HEAD_COUNT), minval=2.5, maxval=4.0)
    fast_level = -jax.random.uniform(key_tensor[2], (SEQUENCE_COUNT, QUERY_HEAD_COUNT), minval=6.0, maxval=7.5)
    base_level = jnp.where(fast_heads, fast_level, slow_level)
    block_count = TOKEN_LENGTH // TOK_DEV
    shifts = jax.random.uniform(key_tensor[3], (SEQUENCE_COUNT, QUERY_HEAD_COUNT, block_count), minval=-0.7, maxval=0.7)
    shifts = jnp.repeat(shifts, TOK_DEV, axis=2)
    rough_part = jax.random.uniform(key_tensor[4], (SEQUENCE_COUNT, QUERY_HEAD_COUNT, TOKEN_LENGTH), minval=-1.0, maxval=1.0)
    tier_levels = base_level[:, :, None] + shifts + rough_part
    stretch_places = jax.random.randint(key_tensor[5], (SEQUENCE_COUNT, QUERY_HEAD_COUNT, 4), 0, TOKEN_LENGTH)
    stretch_matches = jnp.any(jnp.arange(TOKEN_LENGTH)[None, None, :, None] == stretch_places[:, :, None, :], axis=3)
    stretch_groups = jax.random.uniform(key_tensor[6], (SEQUENCE_COUNT, QUERY_HEAD_COUNT, TOKEN_LENGTH), minval=-2.0, maxval=0.0)
    tier_levels = jnp.where(stretch_matches, stretch_groups, tier_levels)
    return jnp.transpose(tier_levels, (2, 0, 1)).astype(jnp.float32).astype(jnp.bfloat16)


def steps_of(key, shape, cuts, smallest, high):
    def one(axis_at, shards_of):
        heights = jax.random.uniform(jax.random.fold_in(jax.random.fold_in(key, 6), axis_at), (shards_of,), jnp.float32, smallest / len(cuts), high / len(cuts))
        return jnp.repeat(jnp.exp(heights), shape[axis_at] // shards_of).reshape((-1,) + (1,) * (len(shape) - axis_at - 1))

    level = one(*cuts[0])
    for cut in cuts[1:]:
        level = level * one(*cut)
    return level


def normal_values(stream_key, extent, scale, most, cuts=(), kind=jnp.bfloat16):
    values = jax.random.normal(stream_key, extent, jnp.float32) * scale
    if len(cuts) > 0:
        values = steps_of(stream_key, extent, cuts, -0.22, 0.18) * values
    return jnp.clip(values, min=-most, max=most).astype(kind)


def setup_inputs(seed: int = 0) -> dict:
    seeds = jax.random.split(jax.random.key(seed), 9)
    tokens = normal_values(seeds[0], (TOKEN_LENGTH, SEQUENCE_COUNT, D), 1.0, 6.0, ((0, 16),))
    queries = normal_values(seeds[1], (TOKEN_LENGTH, SEQUENCE_COUNT, QUERY_HEAD_COUNT * HEAD), 2.5, 15.0, ((0, 16), (2, 2)))
    key_values = normal_values(seeds[2], (TOKEN_LENGTH, SEQUENCE_COUNT, KV_HEADS * 2 * HEAD), 1.0, 6.0, ((0, 16), (2, 2)))
    stop_bias = draw_stop_bias(jax.random.fold_in(seeds[8], 71), 0)
    out_proj = normal_values(seeds[4], (QUERY_HEAD_COUNT * HEAD, D), (QUERY_HEAD_COUNT * HEAD // 4) ** -0.5, 0.375, ((0, 2),))
    norm_gain = jnp.clip(1.0 + 0.18 * jax.random.normal(seeds[5], (D,), jnp.float32), 0.1, 1.9)
    up_proj = normal_values(seeds[6], (D, FF), D ** -0.5, 0.125, ((0, 16), (1, 2)))
    down_proj = normal_values(seeds[7], (FF, D), FF ** -0.5, 0.09375, ((0, 2), (1, 16)))
    return {"tokens": tokens, "queries": queries, "key_values": key_values, "stop_bias": stop_bias, "out_proj": out_proj, "norm_gain": norm_gain, "up_proj": up_proj, "down_proj": down_proj}


EPSILON = 1e-06

def rms_scale(residual, gain):
    values = residual.astype(jnp.float32)
    factor = lax.rsqrt(lax.optimization_barrier(jnp.mean(values * values, axis=-1, keepdims=True)) + EPSILON)
    return (values * factor * gain).astype(jnp.bfloat16)

def reference(tokens, queries, key_values, stop_bias, out_proj, norm_gain, up_proj, down_proj):
    total_rows = tokens.shape[0]
    seq_count = tokens.shape[1]
    group_size = QUERY_HEAD_COUNT // KV_HEADS
    block_count = total_rows // TOK_DEV
    query_heads = queries.reshape(total_rows, seq_count, QUERY_HEAD_COUNT, HEAD).transpose(1, 2, 0, 3)
    query_heads = query_heads.reshape(seq_count * QUERY_HEAD_COUNT, total_rows, HEAD)
    kv_pairs = key_values.reshape(total_rows, seq_count, KV_HEADS, 2 * HEAD).transpose(1, 2, 0, 3)
    biases = jnp.transpose(stop_bias, (1, 2, 0)).astype(jnp.float32)
    positions = jnp.arange(total_rows, dtype=jnp.int32)

    def one_head(inputs):
        flat_index, q_head = inputs
        seq_index = flat_index // QUERY_HEAD_COUNT
        head_index = flat_index % QUERY_HEAD_COUNT
        kv_pair = kv_pairs[seq_index, head_index // group_size]
        keys_part = kv_pair[:, :HEAD]
        values_part = kv_pair[:, HEAD:]
        bias_row = biases[seq_index, head_index]
        q_blocks = q_head.reshape(block_count, TOK_DEV, HEAD)

        def one_block(block_inputs):
            number, q_block = block_inputs
            scores = jnp.dot(q_block, jnp.transpose(keys_part), preferred_element_type=jnp.float32) * 0.125 + bias_row[None, :]
            query_pos = number * TOK_DEV + jnp.arange(TOK_DEV, dtype=jnp.int32)
            strict = positions[None, :] < query_pos[:, None]
            log_pass = jnp.where(strict, jax.nn.log_sigmoid(-scores), 0.0)
            after_sum = lax.cumsum(log_pass, axis=1, reverse=True) - log_pass
            weights = jnp.where(strict, jnp.exp(jax.nn.log_sigmoid(scores) + after_sum), 0.0).astype(jnp.bfloat16)
            return jnp.dot(weights, values_part, preferred_element_type=jnp.float32).astype(jnp.bfloat16)
        outputs = lax.map(one_block, (jnp.arange(block_count, dtype=jnp.int32), q_blocks))
        return outputs.reshape(total_rows, HEAD)
    attended = lax.map(one_head, (jnp.arange(seq_count * QUERY_HEAD_COUNT, dtype=jnp.int32), query_heads))
    attended = attended.reshape(seq_count, QUERY_HEAD_COUNT, total_rows, HEAD).transpose(2, 0, 1, 3)
    attended = attended.reshape(total_rows * seq_count, QUERY_HEAD_COUNT * HEAD)
    head_width = QUERY_HEAD_COUNT * HEAD // N_TP
    projected = jnp.zeros((total_rows * seq_count, D), jnp.float32)
    for group_index in range(N_TP):
        lower = group_index * head_width
        partial_value = jnp.dot(attended[:, lower:lower + head_width], out_proj[lower:lower + head_width], preferred_element_type=jnp.float32)
        projected = projected + lax.optimization_barrier(partial_value.astype(jnp.bfloat16)).astype(jnp.float32)
    flat_tokens = tokens.reshape(total_rows * seq_count, D)
    residual = (flat_tokens.astype(jnp.float32) + projected).astype(jnp.bfloat16)
    normed = rms_scale(residual, norm_gain)
    hidden = jnp.square(jax.nn.relu(jnp.dot(normed, up_proj, preferred_element_type=jnp.float32))).astype(jnp.bfloat16)
    unit_width = FF // N_TP
    update = jnp.zeros((total_rows * seq_count, D), jnp.float32)
    for group_index in range(N_TP):
        lower = group_index * unit_width
        partial_value = jnp.dot(hidden[:, lower:lower + unit_width], down_proj[lower:lower + unit_width], preferred_element_type=jnp.float32)
        update = update + lax.optimization_barrier(partial_value.astype(jnp.bfloat16)).astype(jnp.float32)
    result = (residual.astype(jnp.float32) + update).astype(jnp.bfloat16)
    return result.reshape(total_rows, seq_count, D)
```

```python
import math

import jax
import jax.numpy as jnp
from jax import lax
from jax.experimental import pallas as pl
from jax.experimental.pallas import tpu as pltpu
from jax.sharding import PartitionSpec as P

HEAD = 64


EPSILON = 1e-06


def rms_scale(residual, gain):
    values = residual.astype(jnp.float32)
    factor = lax.rsqrt(jnp.mean(values * values, axis=-1, keepdims=True) + EPSILON)
    return (values * factor * gain).astype(jnp.bfloat16)


def sweep_keys(totals, pieces, shard_rows, step_fn):
    kv_rows, bias_rows = pieces
    shards = kv_rows.shape[0] // shard_rows
    group_shards = math.gcd(shards, max(1, 1024 // shard_rows))
    span_rows = group_shards * shard_rows

    def advance(number, running):
        first_row = number * span_rows
        kv_block = lax.dynamic_slice_in_dim(kv_rows, first_row, span_rows, 0)
        bias_block = lax.dynamic_slice_in_dim(bias_rows, first_row, span_rows, 0)
        return step_fn(running, kv_block, bias_block, first_row, group_shards)

    return lax.fori_loop(0, shards // group_shards, advance, totals)


def general_body(tokens, queries, key_values, stop_bias, out_proj, norm_gain, up_proj, down_proj):
    row_count = tokens.shape[0]
    seq_count = tokens.shape[1]
    head_count = queries.shape[2] // HEAD
    kv_count = key_values.shape[2] // (2 * HEAD)
    group_size = head_count // kv_count
    n_shards = lax.axis_size("sp")
    query_start = lax.axis_index("sp") * row_count
    query_pos = query_start + lax.iota(jnp.int32, row_count)
    q_heads = queries.reshape(row_count, seq_count, kv_count, group_size, HEAD).transpose(
        1, 2, 3, 0, 4
    )
    q_heads = q_heads.reshape(seq_count, kv_count, group_size * row_count, HEAD)

    def stick_block(kv_block, bias_block, key_start):
        span_rows = kv_block.shape[0]
        key_pairs = kv_block.reshape(span_rows, seq_count, kv_count, 2 * HEAD)
        keys_part = key_pairs[..., :HEAD]
        values_part = key_pairs[..., HEAD:]
        scores = (
            jnp.einsum("bgmd,sbgd->bgms", q_heads, keys_part, preferred_element_type=jnp.float32)
            * 0.125
        )
        bias_float = jnp.transpose(bias_block, (1, 2, 0)).astype(jnp.float32)
        scores = (
            scores.reshape(seq_count, head_count, row_count, span_rows) + bias_float[:, :, None, :]
        )
        key_pos = key_start + lax.iota(jnp.int32, span_rows)
        strict = key_pos[None, :] < query_pos[:, None]
        log_pass = jnp.where(strict, jax.nn.log_sigmoid(-scores), 0.0)
        return (scores, strict, log_pass, values_part)

    def weigh(scores, strict, after_sum, values_part):
        span_rows = scores.shape[3]
        weights = jnp.where(strict, jnp.exp(jax.nn.log_sigmoid(scores) + after_sum), 0.0).astype(
            jnp.bfloat16
        )
        weights = weights.reshape(seq_count, kv_count, group_size * row_count, span_rows)
        return jnp.einsum(
            "bgms,sbgd->bgmd", weights, values_part, preferred_element_type=jnp.float32
        )

    empty_out = jnp.zeros((seq_count, kv_count, group_size * row_count, HEAD), jnp.float32)

    def sum_step(sums_table, kv_block, bias_block, key_start, shard_group):

        def sum_compute(table_in):
            scores, strict, log_pass, values_part = stick_block(kv_block, bias_block, key_start)
            block_sums = log_pass.reshape(
                seq_count, head_count, row_count, shard_group, row_count
            ).sum(axis=4)
            slot_index = key_start // row_count
            current = lax.dynamic_slice_in_dim(table_in, slot_index, shard_group, 0)
            return lax.dynamic_update_slice_in_dim(
                table_in, current + jnp.transpose(block_sums, (3, 0, 1, 2)), slot_index, 0
            )

        return lax.cond(
            key_start < query_start + row_count, sum_compute, lambda table_in: table_in, sums_table
        )

    empty_table = jnp.zeros((n_shards, seq_count, head_count, row_count), jnp.float32)
    sums_table = sweep_keys(
        empty_table,
        (
            lax.all_gather(key_values, "sp", axis=0, tiled=True),
            lax.all_gather(stop_bias, "sp", axis=0, tiled=True),
        ),
        row_count,
        sum_step,
    )
    offsets = lax.cumsum(sums_table, axis=0, reverse=True) - sums_table

    def out_step(outputs, kv_block, bias_block, key_start, shard_group):

        def out_compute(running):
            scores, strict, log_pass, values_part = stick_block(kv_block, bias_block, key_start)
            span_rows = kv_block.shape[0]
            split_pass = log_pass.reshape(seq_count, head_count, row_count, shard_group, row_count)
            within = lax.cumsum(split_pass, axis=4, reverse=True) - split_pass
            carried = lax.dynamic_slice_in_dim(offsets, key_start // row_count, shard_group, 0)
            carried = jnp.transpose(carried, (1, 2, 3, 0))[..., None]
            after_sum = (within + carried).reshape(seq_count, head_count, row_count, span_rows)
            return running + weigh(scores, strict, after_sum, values_part)

        return lax.cond(
            key_start < query_start + row_count, out_compute, lambda running: running, outputs
        )

    accum_out = sweep_keys(
        empty_out,
        (
            lax.all_gather(key_values, "sp", axis=0, tiled=True),
            lax.all_gather(stop_bias, "sp", axis=0, tiled=True),
        ),
        row_count,
        out_step,
    )
    attended = accum_out.reshape(seq_count, kv_count, group_size, row_count, HEAD).transpose(
        3, 0, 1, 2, 4
    )
    attended = attended.reshape(row_count * seq_count, head_count * HEAD).astype(jnp.bfloat16)
    share_tokens = row_count // lax.axis_size("tp")
    share_rows = share_tokens * seq_count
    tp_index = lax.axis_index("tp")
    projected = lax.psum(
        jnp.dot(attended, out_proj, preferred_element_type=jnp.float32).astype(jnp.bfloat16), "tp"
    ).astype(jnp.float32)
    flat_tokens = tokens.reshape(row_count * seq_count, tokens.shape[2])
    residual = (flat_tokens.astype(jnp.float32) + projected).astype(jnp.bfloat16)
    normed = rms_scale(residual, norm_gain)
    residual_share = lax.dynamic_slice_in_dim(residual, tp_index * share_rows, share_rows, 0)
    up_values = jnp.dot(
        normed,
        lax.all_gather(up_proj, "sp", axis=0, tiled=True),
        preferred_element_type=jnp.float32,
    )
    hidden = jnp.square(jax.nn.relu(up_values)).astype(jnp.bfloat16)
    partial_terms = jnp.dot(
        hidden,
        lax.all_gather(down_proj, "sp", axis=1, tiled=True),
        preferred_element_type=jnp.float32,
    )
    update = lax.psum_scatter(
        partial_terms.astype(jnp.bfloat16), "tp", scatter_dimension=0, tiled=True
    ).astype(jnp.float32)
    result = (residual_share.astype(jnp.float32) + update).astype(jnp.bfloat16)
    return result.reshape(share_tokens, seq_count, result.shape[1])


MESH = pl.DeviceIdType.MESH
LO = 4
LANES = 128
F32 = jnp.float32
BF16 = jnp.bfloat16


def remote(src, dst, send, recv, sp, tp):
    return pltpu.make_async_remote_copy(
        src_ref=src,
        dst_ref=dst,
        send_sem=send,
        recv_sem=recv,
        device_id={"sp": sp, "tp": tp},
        device_id_type=MESH,
    )


def dot_nt(a, b):
    return lax.dot_general(a, b, (((1,), (1,)), ((), ())), preferred_element_type=F32)


def dot_tn(a, b):
    return lax.dot_general(a, b, (((0,), (0,)), ((), ())), preferred_element_type=F32)


def layer_kernel(
    HI,
    G,
    tok_ref,
    q_ref,
    kvb_ref,
    wo_ref,
    gain_ref,
    up_ref,
    dn_ref,
    out_ref,
    kv_buf,
    up_buf,
    dn_buf,
    q_buf,
    tri_buf,
    carry,
    acc,
    att_buf,
    pj_buf,
    pj_in,
    res_buf,
    n_buf,
    hid_buf,
    ps_buf,
    pr_buf,
    kv_sz,
    kv_sp,
    kv_recv,
    wz_send,
    wp_send,
    up_recv,
    dn_recv,
    pj_send,
    pj_recv,
    n_send,
    nf_send,
    n_recv,
    p_send,
    p_recv,
):
    s = lax.axis_index("sp")
    c = lax.axis_index("tp")
    hi = s // LO
    lo = s % LO
    lo1 = lo + 1 - 2 * (lo % 2)
    lo2 = (lo + 2) % LO
    lo3 = (lo1 + 2) % LO
    other = 1 - c
    T = q_ref.shape[0]
    H = T // 2
    D = tok_ref.shape[1]
    R = up_ref.shape[0]
    CH = up_buf.shape[1]
    KW = G * LANES
    PL = LO * T

    barrier = pltpu.get_barrier_semaphore()
    for p in (lo1, lo2, lo3):
        pl.semaphore_signal(barrier, inc=1, device_id={"sp": hi * LO + p, "tp": c}, device_id_type=MESH)
    pl.semaphore_signal(barrier, inc=1, device_id={"sp": s, "tp": other}, device_id_type=MESH)
    for dz in range(1, HI):
        far = ((hi + dz) % HI) * LO + lo
        for core in range(2):
            pl.semaphore_signal(barrier, inc=1, device_id={"sp": far, "tp": core}, device_id_type=MESH)
    pl.semaphore_wait(barrier, 4 + 2 * (HI - 1))

    def kv_up(hp):
        return remote(
            kvb_ref, kv_buf.at[pl.ds(s * T, T)], kv_sz.at[hp], kv_recv.at[s], hp * LO + lo, c
        )

    def kv_flat(hp, k, src):
        j = hp * LO + lo
        peer = (lo1, lo2, lo3)[k]
        return remote(
            src, kv_buf.at[pl.ds(j * T, T)], kv_sp.at[hp * 3 + k], kv_recv.at[j], hi * LO + peer, c
        )

    def kv_wait(j):
        block = kv_buf.at[pl.ds(j * T, T)]
        remote(block, block, kv_sz.at[0], kv_recv.at[j], s, other).wait_recv()

    def w_far(dz):
        hp = (hi + dz) % HI
        far = hp * LO + lo
        return (
            remote(
                up_ref.at[:, pl.ds(pl.multiple_of(hp * CH, LANES), CH)],
                up_buf.at[pl.ds(s * R, R)],
                wz_send.at[2 * dz],
                up_recv.at[s],
                far,
                c,
            ),
            remote(
                dn_ref.at[pl.ds(hp * CH, CH)],
                dn_buf.at[s],
                wz_send.at[2 * dz + 1],
                dn_recv.at[s],
                far,
                c,
            ),
        )

    def up_at(j):
        return up_buf.at[pl.ds(j * R, R)]

    def up_wait(j):
        remote(up_at(j), up_at(j), wz_send.at[0], up_recv.at[j], s, other).wait_recv()

    def dn_wait(j):
        remote(dn_buf.at[j], dn_buf.at[j], wz_send.at[0], dn_recv.at[j], s, other).wait_recv()

    def w_flat(dz):
        j = ((hi - dz + HI) % HI) * LO + lo
        if dz == 0:
            up_src = up_ref.at[:, pl.ds(pl.multiple_of(hi * CH, LANES), CH)]
            dn_src = dn_ref.at[pl.ds(hi * CH, CH)]
        else:
            up_src = up_at(j)
            dn_src = dn_buf.at[j]
        copies = []
        for k, peer in enumerate((lo1, lo2)):
            far = hi * LO + peer
            copies.append(remote(up_src, up_at(j), wp_send.at[6 * dz + 2 * k], up_recv.at[j], far, c))
            copies.append(
                remote(dn_src, dn_buf.at[j], wp_send.at[6 * dz + 2 * k + 1], dn_recv.at[j], far, c)
            )
        return copies

    def w_diag(dz):
        row = ((hi - dz + HI) % HI) * LO
        return (
            remote(
                up_at(row + lo1),
                up_at(row + lo1),
                wp_send.at[6 * dz + 4],
                up_recv.at[row + lo1],
                hi * LO + lo2,
                c,
            ),
            remote(
                dn_buf.at[row + lo2],
                dn_buf.at[row + lo2],
                wp_send.at[6 * dz + 5],
                dn_recv.at[row + lo2],
                hi * LO + lo1,
                c,
            ),
        )

    for hp in range(HI):

        @pl.when(hp > hi)
        def _():
            kv_up(hp).start()

    for hp in range(HI):

        @pl.when(hp == hi)
        def _():
            for k in range(3):
                kv_flat(hp, k, kvb_ref).start()

    for dz in range(1, HI):
        for copy in w_far(dz):
            copy.start()

    kv_buf[pl.ds(s * T, T), :] = kvb_ref[...]
    up_buf[pl.ds(s * R, R), :] = up_ref[:, pl.ds(pl.multiple_of(hi * CH, LANES), CH)]
    dn_buf[s] = dn_ref[pl.ds(hi * CH, CH), :]
    row_id = lax.broadcasted_iota(jnp.int32, (PL, PL), 0)
    col_id = lax.broadcasted_iota(jnp.int32, (PL, PL), 1)
    tri_buf[...] = jnp.where(col_id > row_id, 1.0, 0.0).astype(BF16)
    lane = lax.broadcasted_iota(jnp.int32, (T, LANES), 1)
    low = lane < HEAD
    for g in range(G):
        qg = q_ref[:, g * LANES : (g + 1) * LANES].astype(F32) * 0.125
        first = jnp.where(low, qg, 0.0)
        second = jnp.where(low, pltpu.roll(qg, HEAD, 1), 0.0)
        q_buf[g] = jnp.concatenate([first, second], axis=0).astype(BF16)
    carry[...] = jnp.zeros_like(carry)
    acc[...] = jnp.zeros_like(acc)

    for hp in range(HI - 1):

        @pl.when(hp < hi)
        def _():
            kv_wait(hp * LO + lo)
            for k in range(3):
                kv_flat(hp, k, kv_buf.at[pl.ds((hp * LO + lo) * T, T)]).start()

    for copy in w_flat(0):
        copy.start()

    sel_row = lax.broadcasted_iota(jnp.int32, (LANES, LANES), 0) // HEAD
    sel_lane = lax.broadcasted_iota(jnp.int32, (LANES, LANES), 1)
    key_row = lax.broadcasted_iota(jnp.int32, (PL, LANES), 0)
    query_pos = s * T + lax.broadcasted_iota(jnp.int32, (PL, LANES), 1) % T

    def attend(plane):
        for p in (lo1, lo2, lo3):
            kv_wait(plane * LO + p)
        rows = pl.ds(plane * PL, PL)
        bias = kv_buf[rows, KW : KW + LANES]
        strict = plane * PL + key_row < query_pos
        for g in range(G):
            kv = kv_buf[rows, g * LANES : (g + 1) * LANES]
            pick = jnp.where(sel_lane == 2 * g + sel_row, 1.0, 0.0).astype(BF16)
            scores = dot_nt(kv, q_buf[g]) + dot_nt(bias, pick)
            soft = jnp.maximum(scores, 0.0) + jnp.log(1.0 + jnp.exp(-jnp.abs(scores)))
            log_pass = jnp.where(strict, -soft, 0.0)
            top = log_pass.astype(BF16)
            rest = (log_pass - top.astype(F32)).astype(BF16)
            after = jnp.dot(tri_buf[...], top, preferred_element_type=F32) + jnp.dot(
                tri_buf[...], rest, preferred_element_type=F32
            )
            held = carry[g]
            weights = jnp.where(strict, jnp.exp(scores - soft + after + held), 0.0).astype(BF16)
            acc[g] += dot_tn(weights, kv)
            carry[g] = held + after[0:1] + log_pass[0:1]

    for k in range(HI):

        @pl.when(k <= hi)
        def _():
            attend(hi - k)

        if k + 1 < HI:
            j = ((hi - k - 1 + HI) % HI) * LO + lo
            up_wait(j)
            dn_wait(j)
            for copy in w_flat(k + 1):
                copy.start()

    for g in range(G):
        a0 = pltpu.roll(acc[g, 0:T, :], HEAD, 1)
        a1 = acc[g, T : 2 * T, :]
        att_buf[:, g * LANES : (g + 1) * LANES] = jnp.where(low, a0, a1).astype(BF16)
    att = att_buf[...]
    wide = 512 if D % 512 == 0 else LANES

    @pl.loop(0, D // wide)
    def _(i):
        cols = pl.ds(pl.multiple_of(i * wide, wide), wide)
        part = jnp.dot(att, wo_ref[:, cols], preferred_element_type=F32)
        pj_buf[:, cols] = part.astype(BF16)

    pj_copy = remote(pj_buf.at[pl.ds(other * H, H)], pj_in, pj_send, pj_recv, s, other)
    pj_copy.start()
    pj_copy.wait()
    mine = pl.ds(c * H, H)
    total = pj_buf[mine, :].astype(F32) + pj_in[...].astype(F32)
    residual = (tok_ref[mine, :].astype(F32) + total).astype(BF16)
    res_buf[...] = residual
    values = residual.astype(F32)
    factor = lax.rsqrt(jnp.mean(values * values, axis=-1, keepdims=True) + EPSILON)
    me = hi * 2 + c

    def n_at(i):
        return n_buf.at[pl.ds(i * H, H)]

    n_buf[pl.ds(me * H, H), :] = (values * factor * gain_ref[...]).astype(BF16)

    def n_out(dz):
        hp = (hi + dz) % HI
        return remote(n_at(me), n_at(me), n_send.at[dz], n_recv.at[me], hp * LO + lo, c)

    def n_pass(dz):
        i = ((hi - dz + HI) % HI) * 2 + c
        return remote(n_at(i), n_at(i), nf_send.at[dz], n_recv.at[i], s, other)

    def n_wait(i):
        remote(n_at(i), n_at(i), nf_send.at[0], n_recv.at[i], s, other).wait_recv()

    for dz in range(1, HI):
        n_out(dz).start()
    n_pass(0).start()

    for dz in range(HI):
        row = ((hi - dz + HI) % HI) * LO
        up_wait(row + lo1)
        dn_wait(row + lo2)
        for copy in w_diag(dz):
            copy.start()
    for dz in range(1, HI):
        n_wait(((hi - dz + HI) % HI) * 2 + c)
        n_pass(dz).start()
    for dz in range(HI):
        n_wait(((hi - dz + HI) % HI) * 2 + other)
    for dz in range(HI):
        row = ((hi - dz + HI) % HI) * LO
        up_wait(row + lo2)
        up_wait(row + lo3)
        dn_wait(row + lo1)
        dn_wait(row + lo3)

    step = 256 if CH % 256 == 0 else LANES
    for i in range(CH // step):
        cols = slice(i * step, (i + 1) * step)
        raw = jnp.maximum(jnp.dot(n_buf[...], up_buf[:, cols], preferred_element_type=F32), 0.0)
        hid_buf[:, cols] = (raw * raw).astype(BF16)
    W = dn_ref.shape[1]

    @pl.loop(0, HI * LO)
    def _(j):
        cols = pl.ds(pl.multiple_of(j * W, LANES), W)
        part = jnp.dot(hid_buf[...], dn_buf[j], preferred_element_type=F32)
        ps_buf[:, cols] = part.astype(BF16)

    def p_out(dz, dc):
        i = ((hi + dz) % HI) * 2 + (c + dc) % 2
        return remote(
            ps_buf.at[pl.ds(i * H, H)],
            pr_buf.at[me],
            p_send.at[2 * dz + dc],
            p_recv.at[me],
            ((hi + dz) % HI) * LO + lo,
            (c + dc) % 2,
        )

    pairs = [(dz, dc) for dz in range(HI) for dc in range(2) if dz + dc > 0]
    for dz, dc in pairs:
        p_out(dz, dc).start()
    update = ps_buf[pl.ds(me * H, H), :].astype(F32)
    for dz, dc in pairs:
        i = ((hi - dz + HI) % HI) * 2 + (c + dc) % 2
        remote(pr_buf.at[i], pr_buf.at[i], p_send.at[0], p_recv.at[i], s, other).wait_recv()
        update = update + pr_buf[i].astype(F32)
    out_ref[...] = (res_buf[...].astype(F32) + update).astype(BF16)

    for hp in range(HI):

        @pl.when(hp > hi)
        def _():
            kv_up(hp).wait_send()

        @pl.when(hp <= hi)
        def _():
            for k in range(3):
                kv_flat(hp, k, kvb_ref).wait_send()

    for dz in range(HI):
        if dz > 0:
            for copy in w_far(dz):
                copy.wait_send()
            n_out(dz).wait_send()
        n_pass(dz).wait_send()
        for copy in w_flat(dz):
            copy.wait_send()
        for copy in w_diag(dz):
            copy.wait_send()
    for dz, dc in pairs:
        p_out(dz, dc).wait_send()


def fits(tokens, queries, key_values, stop_bias, up_proj, down_proj):
    sp = lax.axis_size("sp")
    rows, seqs, heads = stop_bias.shape
    hidden = up_proj.shape[1]
    return (
        lax.axis_size("tp") == 2
        and sp % LO == 0
        and seqs == 1
        and heads <= LANES
        and queries.shape[2] == heads * HEAD
        and key_values.shape[2] == heads * HEAD
        and 2 * HEAD == LANES
        and 2 * rows == LANES
        and hidden % (sp // LO * LANES) == 0
        and down_proj.shape[1] % LANES == 0
        and up_proj.shape[0] % 16 == 0
        and tokens.shape[2] % LANES == 0
    )


def body(tokens, queries, key_values, stop_bias, out_proj, norm_gain, up_proj, down_proj):
    if not fits(tokens, queries, key_values, stop_bias, up_proj, down_proj):
        return general_body(
            tokens, queries, key_values, stop_bias, out_proj, norm_gain, up_proj, down_proj
        )
    sp = lax.axis_size("sp")
    HI = sp // LO
    T, _, D = tokens.shape
    H = T // 2
    heads = stop_bias.shape[2]
    G = heads // 2
    R, hidden = up_proj.shape
    CH = hidden // HI
    W = down_proj.shape[1]
    kvb = jnp.concatenate(
        [
            key_values.reshape(T, key_values.shape[2]),
            jnp.pad(stop_bias.reshape(T, heads), ((0, 0), (0, LANES - heads))),
        ],
        axis=1,
    )
    KB = kvb.shape[1]
    vmem = pl.BlockSpec(memory_space=pltpu.VMEM)
    dma = pltpu.SemaphoreType.DMA
    out = pl.pallas_call(
        lambda *refs: layer_kernel(HI, G, *refs),
        out_shape=jax.ShapeDtypeStruct((H, D), BF16),
        in_specs=[vmem] * 7,
        out_specs=vmem,
        scratch_shapes=[
            pltpu.VMEM((sp * T, KB), BF16),
            pltpu.VMEM((sp * R, CH), BF16),
            pltpu.VMEM((sp, CH, W), BF16),
            pltpu.VMEM((G, LANES, LANES), BF16),
            pltpu.VMEM((LO * T, LO * T), BF16),
            pltpu.VMEM((G, 1, LANES), F32),
            pltpu.VMEM((G, LANES, LANES), F32),
            pltpu.VMEM((T, G * LANES), BF16),
            pltpu.VMEM((T, D), BF16),
            pltpu.VMEM((H, D), BF16),
            pltpu.VMEM((H, D), BF16),
            pltpu.VMEM((HI * T, D), BF16),
            pltpu.VMEM((HI * T, CH), BF16),
            pltpu.VMEM((HI * T, D), BF16),
            pltpu.VMEM((HI * 2, H, D), BF16),
            dma((HI,)),
            dma((HI * 3,)),
            dma((sp,)),
            dma((HI * 2,)),
            dma((HI * 6,)),
            dma((sp,)),
            dma((sp,)),
            dma,
            dma,
            dma((HI,)),
            dma((HI,)),
            dma((HI * 2,)),
            dma((HI * 2,)),
            dma((HI * 2,)),
        ],
        compiler_params=pltpu.CompilerParams(
            collective_id=0, has_side_effects=True, vmem_limit_bytes=56 * 1024 * 1024
        ),
        name="layer",
    )(
        tokens.reshape(T, D),
        queries.reshape(T, queries.shape[2]),
        kvb,
        out_proj,
        norm_gain.reshape(1, D),
        up_proj,
        down_proj,
    )
    return out.reshape(H, 1, D)


def solution(mesh):
    return jax.shard_map(
        body,
        mesh=mesh,
        in_specs=(
            P("sp", None, None),
            P("sp", None, "tp"),
            P("sp", None, "tp"),
            P("sp", None, "tp"),
            P("tp", None),
            P(),
            P("sp", "tp"),
            P("tp", "sp"),
        ),
        out_specs=P(("sp", "tp"), None, None),
        check_vma=False,
    )
```

```python
import math

import jax
import jax.numpy as jnp
from jax import lax
from jax.experimental import pallas as pl
from jax.experimental.pallas import tpu as pltpu
from jax.sharding import PartitionSpec as P

HEAD = 64


EPSILON = 1e-06


def rms_scale(residual, gain):
    values = residual.astype(jnp.float32)
    factor = lax.rsqrt(jnp.mean(values * values, axis=-1, keepdims=True) + EPSILON)
    return (values * factor * gain).astype(jnp.bfloat16)


def sweep_keys(totals, pieces, shard_rows, step_fn):
    kv_rows, bias_rows = pieces
    shards = kv_rows.shape[0] // shard_rows
    group_shards = math.gcd(shards, max(1, 1024 // shard_rows))
    span_rows = group_shards * shard_rows

    def advance(number, running):
        first_row = number * span_rows
        kv_block = lax.dynamic_slice_in_dim(kv_rows, first_row, span_rows, 0)
        bias_block = lax.dynamic_slice_in_dim(bias_rows, first_row, span_rows, 0)
        return step_fn(running, kv_block, bias_block, first_row, group_shards)

    return lax.fori_loop(0, shards // group_shards, advance, totals)


def general_body(tokens, queries, key_values, stop_bias, out_proj, norm_gain, up_proj, down_proj):
    row_count = tokens.shape[0]
    seq_count = tokens.shape[1]
    head_count = queries.shape[2] // HEAD
    kv_count = key_values.shape[2] // (2 * HEAD)
    group_size = head_count // kv_count
    n_shards = lax.axis_size("sp")
    query_start = lax.axis_index("sp") * row_count
    query_pos = query_start + lax.iota(jnp.int32, row_count)
    q_heads = queries.reshape(row_count, seq_count, kv_count, group_size, HEAD).transpose(
        1, 2, 3, 0, 4
    )
    q_heads = q_heads.reshape(seq_count, kv_count, group_size * row_count, HEAD)

    def stick_block(kv_block, bias_block, key_start):
        span_rows = kv_block.shape[0]
        key_pairs = kv_block.reshape(span_rows, seq_count, kv_count, 2 * HEAD)
        keys_part = key_pairs[..., :HEAD]
        values_part = key_pairs[..., HEAD:]
        scores = (
            jnp.einsum("bgmd,sbgd->bgms", q_heads, keys_part, preferred_element_type=jnp.float32)
            * 0.125
        )
        bias_float = jnp.transpose(bias_block, (1, 2, 0)).astype(jnp.float32)
        scores = (
            scores.reshape(seq_count, head_count, row_count, span_rows) + bias_float[:, :, None, :]
        )
        key_pos = key_start + lax.iota(jnp.int32, span_rows)
        strict = key_pos[None, :] < query_pos[:, None]
        log_pass = jnp.where(strict, jax.nn.log_sigmoid(-scores), 0.0)
        return (scores, strict, log_pass, values_part)

    def weigh(scores, strict, after_sum, values_part):
        span_rows = scores.shape[3]
        weights = jnp.where(strict, jnp.exp(jax.nn.log_sigmoid(scores) + after_sum), 0.0).astype(
            jnp.bfloat16
        )
        weights = weights.reshape(seq_count, kv_count, group_size * row_count, span_rows)
        return jnp.einsum(
            "bgms,sbgd->bgmd", weights, values_part, preferred_element_type=jnp.float32
        )

    empty_out = jnp.zeros((seq_count, kv_count, group_size * row_count, HEAD), jnp.float32)

    def sum_step(sums_table, kv_block, bias_block, key_start, shard_group):

        def sum_compute(table_in):
            scores, strict, log_pass, values_part = stick_block(kv_block, bias_block, key_start)
            block_sums = log_pass.reshape(
                seq_count, head_count, row_count, shard_group, row_count
            ).sum(axis=4)
            slot_index = key_start // row_count
            current = lax.dynamic_slice_in_dim(table_in, slot_index, shard_group, 0)
            return lax.dynamic_update_slice_in_dim(
                table_in, current + jnp.transpose(block_sums, (3, 0, 1, 2)), slot_index, 0
            )

        return lax.cond(
            key_start < query_start + row_count, sum_compute, lambda table_in: table_in, sums_table
        )

    empty_table = jnp.zeros((n_shards, seq_count, head_count, row_count), jnp.float32)
    sums_table = sweep_keys(
        empty_table,
        (
            lax.all_gather(key_values, "sp", axis=0, tiled=True),
            lax.all_gather(stop_bias, "sp", axis=0, tiled=True),
        ),
        row_count,
        sum_step,
    )
    offsets = lax.cumsum(sums_table, axis=0, reverse=True) - sums_table

    def out_step(outputs, kv_block, bias_block, key_start, shard_group):

        def out_compute(running):
            scores, strict, log_pass, values_part = stick_block(kv_block, bias_block, key_start)
            span_rows = kv_block.shape[0]
            split_pass = log_pass.reshape(seq_count, head_count, row_count, shard_group, row_count)
            within = lax.cumsum(split_pass, axis=4, reverse=True) - split_pass
            carried = lax.dynamic_slice_in_dim(offsets, key_start // row_count, shard_group, 0)
            carried = jnp.transpose(carried, (1, 2, 3, 0))[..., None]
            after_sum = (within + carried).reshape(seq_count, head_count, row_count, span_rows)
            return running + weigh(scores, strict, after_sum, values_part)

        return lax.cond(
            key_start < query_start + row_count, out_compute, lambda running: running, outputs
        )

    accum_out = sweep_keys(
        empty_out,
        (
            lax.all_gather(key_values, "sp", axis=0, tiled=True),
            lax.all_gather(stop_bias, "sp", axis=0, tiled=True),
        ),
        row_count,
        out_step,
    )
    attended = accum_out.reshape(seq_count, kv_count, group_size, row_count, HEAD).transpose(
        3, 0, 1, 2, 4
    )
    attended = attended.reshape(row_count * seq_count, head_count * HEAD).astype(jnp.bfloat16)
    share_tokens = row_count // lax.axis_size("tp")
    share_rows = share_tokens * seq_count
    tp_index = lax.axis_index("tp")
    projected = lax.psum(
        jnp.dot(attended, out_proj, preferred_element_type=jnp.float32).astype(jnp.bfloat16), "tp"
    ).astype(jnp.float32)
    flat_tokens = tokens.reshape(row_count * seq_count, tokens.shape[2])
    residual = (flat_tokens.astype(jnp.float32) + projected).astype(jnp.bfloat16)
    normed = rms_scale(residual, norm_gain)
    residual_share = lax.dynamic_slice_in_dim(residual, tp_index * share_rows, share_rows, 0)
    up_values = jnp.dot(
        normed,
        lax.all_gather(up_proj, "sp", axis=0, tiled=True),
        preferred_element_type=jnp.float32,
    )
    hidden = jnp.square(jax.nn.relu(up_values)).astype(jnp.bfloat16)
    partial_terms = jnp.dot(
        hidden,
        lax.all_gather(down_proj, "sp", axis=1, tiled=True),
        preferred_element_type=jnp.float32,
    )
    update = lax.psum_scatter(
        partial_terms.astype(jnp.bfloat16), "tp", scatter_dimension=0, tiled=True
    ).astype(jnp.float32)
    result = (residual_share.astype(jnp.float32) + update).astype(jnp.bfloat16)
    return result.reshape(share_tokens, seq_count, result.shape[1])


MESH = pl.DeviceIdType.MESH
LO = 4
LANES = 128
F32 = jnp.float32
BF16 = jnp.bfloat16


def remote(src, dst, send, recv, sp, tp):
    return pltpu.make_async_remote_copy(
        src_ref=src,
        dst_ref=dst,
        send_sem=send,
        recv_sem=recv,
        device_id={"sp": sp, "tp": tp},
        device_id_type=MESH,
    )


def dot_nt(a, b):
    return lax.dot_general(a, b, (((1,), (1,)), ((), ())), preferred_element_type=F32)


def dot_tn(a, b):
    return lax.dot_general(a, b, (((0,), (0,)), ((), ())), preferred_element_type=F32)


def layer_kernel(
    HI,
    G,
    tok_ref,
    q_ref,
    kvb_ref,
    wo_ref,
    gain_ref,
    up_ref,
    dn_ref,
    out_ref,
    kv_buf,
    up_buf,
    dn_buf,
    q_buf,
    tri_buf,
    carry,
    acc,
    att_buf,
    pj_buf,
    pj_in,
    res_buf,
    n_buf,
    hid_buf,
    ps_buf,
    x_in,
    xs_buf,
    pr_buf,
    kv_sz,
    kv_sp,
    kv_recv,
    kv_half,
    wz_send,
    up_sp,
    up_recv,
    up_half,
    dn_sp,
    dn_recv,
    dn_half,
    pj_send,
    pj_recv,
    n_send,
    nf_send,
    n_recv,
    x_send,
    x_recv,
    p_send,
    p_recv,
):
    s = lax.axis_index("sp")
    c = lax.axis_index("tp")
    hi = s // LO
    lo = s % LO
    lo1 = lo + 1 - 2 * (lo % 2)
    lo2 = (lo + 2) % LO
    lo3 = (lo1 + 2) % LO
    other = 1 - c
    T = q_ref.shape[0]
    H = T // 2
    D = tok_ref.shape[1]
    R = up_ref.shape[0]
    CH = up_buf.shape[1]
    W = dn_ref.shape[1]
    KW = G * LANES
    PL = LO * T
    own_cols = pl.ds(pl.multiple_of(hi * CH, LANES), CH)

    barrier = pltpu.get_barrier_semaphore()
    for p in (lo1, lo2):
        pl.semaphore_signal(barrier, inc=1, device_id={"sp": hi * LO + p, "tp": c}, device_id_type=MESH)
    pl.semaphore_signal(barrier, inc=1, device_id={"sp": s, "tp": other}, device_id_type=MESH)
    for dz in range(1, HI):
        far = ((hi + dz) % HI) * LO + lo
        pl.semaphore_signal(barrier, inc=1, device_id={"sp": far, "tp": c}, device_id_type=MESH)
    pl.semaphore_wait(barrier, 3 + (HI - 1))

    class Piece:
        def __init__(self, view, rows, send, recv, half):
            self.view, self.rows, self.send, self.recv, self.half = view, rows, send, recv, half

        def full(self, j):
            return self.view(j, 0, self.rows)

        def part(self, j, h):
            return self.view(j, h * (self.rows // 2), self.rows // 2)

        def direct(self, z, src=None):
            j = z * LO + lo
            src = self.full(j) if src is None else src
            return [
                remote(src, self.full(j), self.send.at[z * 4 + k], self.recv.at[j], hi * LO + p, c)
                for k, p in enumerate((lo1, lo2))
            ]

        def diag(self, z):
            a, b = z * LO + lo1, z * LO + lo2
            first, last = self.part(a, 0), self.part(b, 1)
            return [
                remote(first, first, self.send.at[z * 4 + 2], self.recv.at[a], hi * LO + lo2, c),
                remote(last, last, self.send.at[z * 4 + 3], self.half.at[z], hi * LO + lo1, c),
            ]

        def arrived(self, ref, sem):
            remote(ref, ref, self.send.at[0], sem, s, other).wait_recv()

        def wait_own(self, z):
            j = z * LO + lo
            self.arrived(self.full(j), self.recv.at[j])

        def wait_direct(self, z):
            for p in (lo1, lo2):
                j = z * LO + p
                self.arrived(self.full(j), self.recv.at[j])

        def wait_diag(self, z):
            j = z * LO + lo3
            self.arrived(self.part(j, 0), self.recv.at[j])
            self.arrived(self.part(j, 1), self.half.at[z])

    kv = Piece(lambda j, r, n: kv_buf.at[pl.ds(j * T + r, n)], T, kv_sp, kv_recv, kv_half)
    up = Piece(lambda j, r, n: up_buf.at[pl.ds(j * R + r, n)], R, up_sp, up_recv, up_half)
    dn = Piece(lambda j, r, n: dn_buf.at[j, pl.ds(r, n)], CH, dn_sp, dn_recv, dn_half)
    up_own = up_ref.at[:, own_cols]
    dn_own = dn_ref.at[pl.ds(hi * CH, CH)]

    def start(copies):
        for copy in copies:
            copy.start()

    def below(dz):
        return (hi - dz + HI) % HI

    def kv_up(hp):
        return remote(kvb_ref, kv.full(s), kv_sz.at[hp], kv_recv.at[s], hp * LO + lo, c)

    def up_far(hp):
        cols = pl.ds(hp * CH, CH)
        return remote(up_ref.at[:, cols], up.full(s), wz_send.at[2 * hp], up_recv.at[s], hp * LO + lo, c)

    def dn_far(hp):
        rows = pl.ds(hp * CH, CH)
        return remote(dn_ref.at[rows], dn.full(s), wz_send.at[2 * hp + 1], dn_recv.at[s], hp * LO + lo, c)

    for hp in range(HI):

        @pl.when(hp > hi)
        def _():
            kv_up(hp).start()

    start(kv.direct(hi, kvb_ref))
    for far in (up_far, dn_far):
        for hp in range(HI - 2, -1, -1):

            @pl.when(hp < hi)
            def _():
                far(hp).start()

    start(up.direct(hi, up_own))
    kv_buf[pl.ds(s * T, T), :] = kvb_ref[...]
    lane = lax.broadcasted_iota(jnp.int32, (T, LANES), 1)
    low = lane < HEAD
    for g in range(G):
        qg = q_ref[:, g * LANES : (g + 1) * LANES].astype(F32) * 0.125
        first = jnp.where(low, qg, 0.0)
        second = jnp.where(low, pltpu.roll(qg, HEAD, 1), 0.0)
        q_buf[g] = jnp.concatenate([first, second], axis=0).astype(BF16)
    row_id = lax.broadcasted_iota(jnp.int32, (PL, PL), 0)
    col_id = lax.broadcasted_iota(jnp.int32, (PL, PL), 1)
    tri_buf[...] = jnp.where(col_id > row_id, 1.0, 0.0).astype(BF16)
    carry[...] = jnp.zeros_like(carry)
    acc[...] = jnp.zeros_like(acc)

    sel_row = lax.broadcasted_iota(jnp.int32, (LANES, LANES), 0) // HEAD
    sel_lane = lax.broadcasted_iota(jnp.int32, (LANES, LANES), 1)
    key_row = lax.broadcasted_iota(jnp.int32, (PL, LANES), 0)
    query_pos = s * T + lax.broadcasted_iota(jnp.int32, (PL, LANES), 1) % T

    def attend(plane):
        rows = pl.ds(plane * PL, PL)
        bias = kv_buf[rows, KW : KW + LANES]
        strict = plane * PL + key_row < query_pos
        for g in range(G):
            pairs = kv_buf[rows, g * LANES : (g + 1) * LANES]
            pick = jnp.where(sel_lane == 2 * g + sel_row, 1.0, 0.0).astype(BF16)
            scores = dot_nt(pairs, q_buf[g]) + dot_nt(bias, pick)
            soft = jnp.maximum(scores, 0.0) + jnp.log(1.0 + jnp.exp(-jnp.abs(scores)))
            log_pass = jnp.where(strict, -soft, 0.0)
            top = log_pass.astype(BF16)
            rest = (log_pass - top.astype(F32)).astype(BF16)
            after = jnp.dot(tri_buf[...], top, preferred_element_type=F32) + jnp.dot(
                tri_buf[...], rest, preferred_element_type=F32
            )
            held = carry[g]
            weights = jnp.where(strict, jnp.exp(scores - soft + after + held), 0.0).astype(BF16)
            acc[g] += dot_tn(weights, pairs)
            carry[g] = held + after[0:1] + log_pass[0:1]

    def column(k):
        @pl.when(k <= hi)
        def _():
            kv.wait_own(hi - k)
            start(kv.direct(hi - k))

    def relay(k):
        @pl.when(k <= hi)
        def _():
            kv.wait_direct(hi - k)
            start(kv.diag(hi - k))

    def look(k):
        @pl.when(k <= hi)
        def _():
            kv.wait_diag(hi - k)
            attend(hi - k)

    def up_column(dz):
        up.wait_own(below(dz))
        start(up.direct(below(dz)))

    def up_relay(dz):
        up.wait_direct(below(dz))
        start(up.diag(below(dz)))

    def dn_column(dz):
        dn.wait_own(below(dz))
        start(dn.direct(below(dz)))

    def dn_relay(dz):
        dn.wait_direct(below(dz))
        start(dn.diag(below(dz)))

    for k in range(1, HI):
        column(k)
        relay(k - 1)
        if k == 1:
            for far in (up_far, dn_far):
                for hp in range(1, HI):

                    @pl.when(hp > hi)
                    def _():
                        far(hp).start()

            up_buf[pl.ds(s * R, R), :] = up_ref[:, own_cols]
            dn_buf[s] = dn_ref[pl.ds(hi * CH, CH), :]
        if k >= 2:
            look(k - 2)
    relay(HI - 1)
    up_column(1)
    up_relay(0)
    if HI >= 2:
        look(HI - 2)
    for dz in range(2, HI):
        up_column(dz)
    start(dn.direct(hi, dn_own))
    look(HI - 1)
    up_relay(1)

    for g in range(G):
        a0 = pltpu.roll(acc[g, 0:T, :], HEAD, 1)
        a1 = acc[g, T : 2 * T, :]
        att_buf[:, g * LANES : (g + 1) * LANES] = jnp.where(low, a0, a1).astype(BF16)
    att = att_buf[...]
    wide = 512 if D % 512 == 0 else LANES
    for i in range(D // wide):
        cols = slice(i * wide, (i + 1) * wide)
        pj_buf[:, cols] = jnp.dot(att, wo_ref[:, cols], preferred_element_type=F32).astype(BF16)

    pj_copy = remote(pj_buf.at[pl.ds(other * H, H)], pj_in, pj_send, pj_recv, s, other)
    pj_copy.start()
    for dz in range(2, HI):
        up_relay(dz)
    pj_copy.wait()
    mine = pl.ds(c * H, H)
    total = pj_buf[mine, :].astype(F32) + pj_in[...].astype(F32)
    residual = (tok_ref[mine, :].astype(F32) + total).astype(BF16)
    res_buf[...] = residual
    values = residual.astype(F32)
    factor = lax.rsqrt(jnp.mean(values * values, axis=-1, keepdims=True) + EPSILON)

    def n_at(z, core):
        return n_buf.at[pl.ds((core * HI + z) * H, H)]

    n_buf[pl.ds((c * HI + hi) * H, H), :] = (values * factor * gain_ref[...]).astype(BF16)

    def n_out(dz):
        hp = (hi + dz) % HI
        return remote(n_at(hi, c), n_at(hi, c), n_send.at[dz], n_recv.at[c * HI + hi], hp * LO + lo, c)

    def n_pass(dz):
        z = below(dz)
        return remote(n_at(z, c), n_at(z, c), nf_send.at[dz], n_recv.at[c * HI + z], s, other)

    def n_wait(z, core):
        ref = n_at(z, core)
        remote(ref, ref, nf_send.at[0], n_recv.at[core * HI + z], s, other).wait_recv()

    for dz in range(1, HI):
        n_out(dz).start()
    n_pass(0).start()
    for dz in range(1, HI):
        dn_column(dz)
    dn_relay(0)
    for dz in range(1, HI):
        n_wait(below(dz), c)
        n_pass(dz).start()
    for dz in range(HI):
        up.wait_diag(below(dz))
    for dz in range(HI):
        n_wait(below(dz), other)

    step = 256 if CH % 256 == 0 else LANES
    for i in range(CH // step):
        cols = slice(i * step, (i + 1) * step)
        raw = jnp.maximum(jnp.dot(n_buf[...], up_buf[:, cols], preferred_element_type=F32), 0.0)
        hid_buf[:, cols] = (raw * raw).astype(BF16)

    half = HI * H

    def x_out(dz):
        z = below(dz)
        rows = pl.ds(other * half, half)
        return remote(ps_buf.at[z, rows], x_in.at[z], x_send.at[dz], x_recv.at[z], s, other)

    def p_out(dz, far):
        z = below(dz)
        hp = (hi + far) % HI
        return remote(
            xs_buf.at[z, pl.ds(hp * H, H)],
            pr_buf.at[hi, z],
            p_send.at[dz * HI + far],
            p_recv.at[hi * HI + z],
            hp * LO + lo,
            c,
        )

    def p_wait(src, z):
        ref = pr_buf.at[src, z]
        remote(ref, ref, p_send.at[0], p_recv.at[src * HI + z], s, other).wait_recv()

    def spread(dz):
        z = below(dz)
        x_in_ref = x_in.at[z]
        remote(x_in_ref, x_in_ref, x_send.at[0], x_recv.at[z], s, other).wait_recv()
        mixed = ps_buf[z, pl.ds(c * half, half), :].astype(F32) + x_in[z].astype(F32)
        xs_buf[z] = mixed.astype(BF16)
        for far in range(1, HI):
            p_out(dz, far).start()

    for dz in range(HI):
        if dz + 1 < HI:
            dn_relay(dz + 1)
        z = below(dz)
        dn.wait_diag(z)
        for q in range(LO):
            part = jnp.dot(hid_buf[...], dn_buf[z * LO + q], preferred_element_type=F32)
            ps_buf[z, :, q * W : (q + 1) * W] = part.astype(BF16)
        x_out(dz).start()
        if dz > 0:
            spread(dz - 1)
    spread(HI - 1)
    CW = LO * W
    for dz in range(HI):
        z = below(dz)
        cols = pl.ds(pl.multiple_of(z * CW, LANES), CW)
        update = xs_buf[z, pl.ds(hi * H, H), :].astype(F32)
        for far in range(1, HI):
            p_wait(below(far), z)
            update = update + pr_buf[below(far), z].astype(F32)
        out_ref[:, cols] = (res_buf[:, cols].astype(F32) + update).astype(BF16)

    for hp in range(HI):

        @pl.when(hp > hi)
        def _():
            kv_up(hp).wait_send()

        @pl.when(hp <= hi)
        def _():
            for copy in kv.direct(hp) + kv.diag(hp):
                copy.wait_send()

        @pl.when(hp != hi)
        def _():
            up_far(hp).wait_send()
            dn_far(hp).wait_send()

        for copy in up.direct(hp) + up.diag(hp) + dn.direct(hp) + dn.diag(hp):
            copy.wait_send()

    for dz in range(HI):
        n_pass(dz).wait_send()
        x_out(dz).wait_send()
        if dz > 0:
            n_out(dz).wait_send()
        for far in range(1, HI):
            p_out(dz, far).wait_send()


def fits(tokens, queries, key_values, stop_bias, up_proj, down_proj):
    sp = lax.axis_size("sp")
    rows, seqs, heads = stop_bias.shape
    hidden = up_proj.shape[1]
    return (
        lax.axis_size("tp") == 2
        and sp % LO == 0
        and sp > LO
        and seqs == 1
        and heads <= LANES
        and queries.shape[2] == heads * HEAD
        and key_values.shape[2] == heads * HEAD
        and 2 * HEAD == LANES
        and 2 * rows == LANES
        and hidden % (sp // LO * LANES) == 0
        and down_proj.shape[1] % LANES == 0
        and up_proj.shape[0] % 16 == 0
        and tokens.shape[2] % LANES == 0
    )


def body(tokens, queries, key_values, stop_bias, out_proj, norm_gain, up_proj, down_proj):
    if not fits(tokens, queries, key_values, stop_bias, up_proj, down_proj):
        return general_body(
            tokens, queries, key_values, stop_bias, out_proj, norm_gain, up_proj, down_proj
        )
    sp = lax.axis_size("sp")
    HI = sp // LO
    T, _, D = tokens.shape
    H = T // 2
    heads = stop_bias.shape[2]
    G = heads // 2
    R, hidden = up_proj.shape
    CH = hidden // HI
    W = down_proj.shape[1]
    kvb = jnp.concatenate(
        [
            key_values.reshape(T, key_values.shape[2]),
            jnp.pad(stop_bias.reshape(T, heads), ((0, 0), (0, LANES - heads))),
        ],
        axis=1,
    )
    KB = kvb.shape[1]
    vmem = pl.BlockSpec(memory_space=pltpu.VMEM)
    dma = pltpu.SemaphoreType.DMA
    out = pl.pallas_call(
        lambda *refs: layer_kernel(HI, G, *refs),
        out_shape=jax.ShapeDtypeStruct((H, D), BF16),
        in_specs=[vmem] * 7,
        out_specs=vmem,
        scratch_shapes=[
            pltpu.VMEM((sp * T, KB), BF16),
            pltpu.VMEM((sp * R, CH), BF16),
            pltpu.VMEM((sp, CH, W), BF16),
            pltpu.VMEM((G, LANES, LANES), BF16),
            pltpu.VMEM((LO * T, LO * T), BF16),
            pltpu.VMEM((G, 1, LANES), F32),
            pltpu.VMEM((G, LANES, LANES), F32),
            pltpu.VMEM((T, G * LANES), BF16),
            pltpu.VMEM((T, D), BF16),
            pltpu.VMEM((H, D), BF16),
            pltpu.VMEM((H, D), BF16),
            pltpu.VMEM((HI * T, D), BF16),
            pltpu.VMEM((HI * T, CH), BF16),
            pltpu.VMEM((HI, HI * T, LO * W), BF16),
            pltpu.VMEM((HI, HI * H, LO * W), BF16),
            pltpu.VMEM((HI, HI * H, LO * W), BF16),
            pltpu.VMEM((HI, HI, H, LO * W), BF16),
            dma((HI,)),
            dma((HI * 4,)),
            dma((sp,)),
            dma((HI,)),
            dma((HI * 2,)),
            dma((HI * 4,)),
            dma((sp,)),
            dma((HI,)),
            dma((HI * 4,)),
            dma((sp,)),
            dma((HI,)),
            dma,
            dma,
            dma((HI,)),
            dma((HI,)),
            dma((HI * 2,)),
            dma((HI,)),
            dma((HI,)),
            dma((HI * HI,)),
            dma((HI * HI,)),
        ],
        compiler_params=pltpu.CompilerParams(
            collective_id=0, has_side_effects=True, vmem_limit_bytes=56 * 1024 * 1024
        ),
        name="layer",
    )(
        tokens.reshape(T, D),
        queries.reshape(T, queries.shape[2]),
        kvb,
        out_proj,
        norm_gain.reshape(1, D),
        up_proj,
        down_proj,
    )
    return out.reshape(H, 1, D)


def solution(mesh):
    return jax.shard_map(
        body,
        mesh=mesh,
        in_specs=(
            P("sp", None, None),
            P("sp", None, "tp"),
            P("sp", None, "tp"),
            P("sp", None, "tp"),
            P("tp", None),
            P(),
            P("sp", "tp"),
            P("tp", "sp"),
        ),
        out_specs=P(("sp", "tp"), None, None),
        check_vma=False,
    )
```

```python
import math

import jax
import jax.numpy as jnp
from jax import lax
from jax.experimental import pallas as pl
from jax.experimental.pallas import tpu as pltpu
from jax.sharding import PartitionSpec as P

HEAD = 64


EPSILON = 1e-06


def rms_scale(residual, gain):
    values = residual.astype(jnp.float32)
    factor = lax.rsqrt(jnp.mean(values * values, axis=-1, keepdims=True) + EPSILON)
    return (values * factor * gain).astype(jnp.bfloat16)


def sweep_keys(totals, pieces, shard_rows, step_fn):
    kv_rows, bias_rows = pieces
    shards = kv_rows.shape[0] // shard_rows
    group_shards = math.gcd(shards, max(1, 1024 // shard_rows))
    span_rows = group_shards * shard_rows

    def advance(number, running):
        first_row = number * span_rows
        kv_block = lax.dynamic_slice_in_dim(kv_rows, first_row, span_rows, 0)
        bias_block = lax.dynamic_slice_in_dim(bias_rows, first_row, span_rows, 0)
        return step_fn(running, kv_block, bias_block, first_row, group_shards)

    return lax.fori_loop(0, shards // group_shards, advance, totals)


def general_body(tokens, queries, key_values, stop_bias, out_proj, norm_gain, up_proj, down_proj):
    row_count = tokens.shape[0]
    seq_count = tokens.shape[1]
    head_count = queries.shape[2] // HEAD
    kv_count = key_values.shape[2] // (2 * HEAD)
    group_size = head_count // kv_count
    n_shards = lax.axis_size("sp")
    query_start = lax.axis_index("sp") * row_count
    query_pos = query_start + lax.iota(jnp.int32, row_count)
    q_heads = queries.reshape(row_count, seq_count, kv_count, group_size, HEAD).transpose(
        1, 2, 3, 0, 4
    )
    q_heads = q_heads.reshape(seq_count, kv_count, group_size * row_count, HEAD)

    def stick_block(kv_block, bias_block, key_start):
        span_rows = kv_block.shape[0]
        key_pairs = kv_block.reshape(span_rows, seq_count, kv_count, 2 * HEAD)
        keys_part = key_pairs[..., :HEAD]
        values_part = key_pairs[..., HEAD:]
        scores = (
            jnp.einsum("bgmd,sbgd->bgms", q_heads, keys_part, preferred_element_type=jnp.float32)
            * 0.125
        )
        bias_float = jnp.transpose(bias_block, (1, 2, 0)).astype(jnp.float32)
        scores = (
            scores.reshape(seq_count, head_count, row_count, span_rows) + bias_float[:, :, None, :]
        )
        key_pos = key_start + lax.iota(jnp.int32, span_rows)
        strict = key_pos[None, :] < query_pos[:, None]
        log_pass = jnp.where(strict, jax.nn.log_sigmoid(-scores), 0.0)
        return (scores, strict, log_pass, values_part)

    def weigh(scores, strict, after_sum, values_part):
        span_rows = scores.shape[3]
        weights = jnp.where(strict, jnp.exp(jax.nn.log_sigmoid(scores) + after_sum), 0.0).astype(
            jnp.bfloat16
        )
        weights = weights.reshape(seq_count, kv_count, group_size * row_count, span_rows)
        return jnp.einsum(
            "bgms,sbgd->bgmd", weights, values_part, preferred_element_type=jnp.float32
        )

    empty_out = jnp.zeros((seq_count, kv_count, group_size * row_count, HEAD), jnp.float32)

    def sum_step(sums_table, kv_block, bias_block, key_start, shard_group):

        def sum_compute(table_in):
            scores, strict, log_pass, values_part = stick_block(kv_block, bias_block, key_start)
            block_sums = log_pass.reshape(
                seq_count, head_count, row_count, shard_group, row_count
            ).sum(axis=4)
            slot_index = key_start // row_count
            current = lax.dynamic_slice_in_dim(table_in, slot_index, shard_group, 0)
            return lax.dynamic_update_slice_in_dim(
                table_in, current + jnp.transpose(block_sums, (3, 0, 1, 2)), slot_index, 0
            )

        return lax.cond(
            key_start < query_start + row_count, sum_compute, lambda table_in: table_in, sums_table
        )

    empty_table = jnp.zeros((n_shards, seq_count, head_count, row_count), jnp.float32)
    sums_table = sweep_keys(
        empty_table,
        (
            lax.all_gather(key_values, "sp", axis=0, tiled=True),
            lax.all_gather(stop_bias, "sp", axis=0, tiled=True),
        ),
        row_count,
        sum_step,
    )
    offsets = lax.cumsum(sums_table, axis=0, reverse=True) - sums_table

    def out_step(outputs, kv_block, bias_block, key_start, shard_group):

        def out_compute(running):
            scores, strict, log_pass, values_part = stick_block(kv_block, bias_block, key_start)
            span_rows = kv_block.shape[0]
            split_pass = log_pass.reshape(seq_count, head_count, row_count, shard_group, row_count)
            within = lax.cumsum(split_pass, axis=4, reverse=True) - split_pass
            carried = lax.dynamic_slice_in_dim(offsets, key_start // row_count, shard_group, 0)
            carried = jnp.transpose(carried, (1, 2, 3, 0))[..., None]
            after_sum = (within + carried).reshape(seq_count, head_count, row_count, span_rows)
            return running + weigh(scores, strict, after_sum, values_part)

        return lax.cond(
            key_start < query_start + row_count, out_compute, lambda running: running, outputs
        )

    accum_out = sweep_keys(
        empty_out,
        (
            lax.all_gather(key_values, "sp", axis=0, tiled=True),
            lax.all_gather(stop_bias, "sp", axis=0, tiled=True),
        ),
        row_count,
        out_step,
    )
    attended = accum_out.reshape(seq_count, kv_count, group_size, row_count, HEAD).transpose(
        3, 0, 1, 2, 4
    )
    attended = attended.reshape(row_count * seq_count, head_count * HEAD).astype(jnp.bfloat16)
    share_tokens = row_count // lax.axis_size("tp")
    share_rows = share_tokens * seq_count
    tp_index = lax.axis_index("tp")
    projected = lax.psum(
        jnp.dot(attended, out_proj, preferred_element_type=jnp.float32).astype(jnp.bfloat16), "tp"
    ).astype(jnp.float32)
    flat_tokens = tokens.reshape(row_count * seq_count, tokens.shape[2])
    residual = (flat_tokens.astype(jnp.float32) + projected).astype(jnp.bfloat16)
    normed = rms_scale(residual, norm_gain)
    residual_share = lax.dynamic_slice_in_dim(residual, tp_index * share_rows, share_rows, 0)
    up_values = jnp.dot(
        normed,
        lax.all_gather(up_proj, "sp", axis=0, tiled=True),
        preferred_element_type=jnp.float32,
    )
    hidden = jnp.square(jax.nn.relu(up_values)).astype(jnp.bfloat16)
    partial_terms = jnp.dot(
        hidden,
        lax.all_gather(down_proj, "sp", axis=1, tiled=True),
        preferred_element_type=jnp.float32,
    )
    update = lax.psum_scatter(
        partial_terms.astype(jnp.bfloat16), "tp", scatter_dimension=0, tiled=True
    ).astype(jnp.float32)
    result = (residual_share.astype(jnp.float32) + update).astype(jnp.bfloat16)
    return result.reshape(share_tokens, seq_count, result.shape[1])


MESH = pl.DeviceIdType.MESH
LO = 4
LANES = 128
F32 = jnp.float32
BF16 = jnp.bfloat16


def remote(src, dst, send, recv, sp, tp):
    return pltpu.make_async_remote_copy(
        src_ref=src,
        dst_ref=dst,
        send_sem=send,
        recv_sem=recv,
        device_id={"sp": sp, "tp": tp},
        device_id_type=MESH,
    )


def dot_nt(a, b):
    return lax.dot_general(a, b, (((1,), (1,)), ((), ())), preferred_element_type=F32)


def dot_tn(a, b):
    return lax.dot_general(a, b, (((0,), (0,)), ((), ())), preferred_element_type=F32)


def layer_kernel(
    HI,
    G,
    tok_ref,
    q_ref,
    kvp_ref,
    bias_ref,
    wo_hbm,
    gain_ref,
    up_ref,
    dn_ref,
    out_ref,
    kvb_ref,
    wo_ref,
    load_sem,
    kv_buf,
    up_buf,
    dn_buf,
    q_buf,
    tri_buf,
    carry,
    acc,
    att_buf,
    pj_buf,
    pj_in,
    res_buf,
    n_buf,
    hid_buf,
    ps_buf,
    x_in,
    xs_buf,
    pr_buf,
    kv_sz,
    kv_sp,
    kv_recv,
    kv_half,
    wz_send,
    up_sp,
    up_recv,
    up_half,
    dn_sp,
    dn_recv,
    dn_half,
    pj_send,
    pj_recv,
    n_send,
    nf_send,
    n_recv,
    x_send,
    x_recv,
    p_send,
    p_recv,
):
    s = lax.axis_index("sp")
    c = lax.axis_index("tp")
    hi = s // LO
    lo = s % LO
    lo1 = lo + 1 - 2 * (lo % 2)
    lo2 = (lo + 2) % LO
    lo3 = (lo1 + 2) % LO
    other = 1 - c
    T = q_ref.shape[0]
    H = T // 2
    D = tok_ref.shape[1]
    R = up_ref.shape[0]
    CH = up_buf.shape[1]
    W = dn_ref.shape[1]
    KW = G * LANES
    PL = LO * T
    own_cols = pl.ds(pl.multiple_of(hi * CH, LANES), CH)

    barrier = pltpu.get_barrier_semaphore()
    for p in (lo1, lo2):
        pl.semaphore_signal(barrier, inc=1, device_id={"sp": hi * LO + p, "tp": c}, device_id_type=MESH)
    pl.semaphore_signal(barrier, inc=1, device_id={"sp": s, "tp": other}, device_id_type=MESH)
    for dz in range(1, HI):
        far = ((hi + dz) % HI) * LO + lo
        pl.semaphore_signal(barrier, inc=1, device_id={"sp": far, "tp": c}, device_id_type=MESH)
    loads = [
        pltpu.make_async_copy(wo_hbm, wo_ref, load_sem.at[0]),
        pltpu.make_async_copy(up_ref.at[:, own_cols], up_buf.at[pl.ds(s * R, R)], load_sem.at[1]),
        pltpu.make_async_copy(dn_ref.at[pl.ds(hi * CH, CH)], dn_buf.at[s], load_sem.at[2]),
    ]
    for load in loads:
        load.start()
    kvb_ref[:, :KW] = kvp_ref[...]
    kvb_ref[:, KW:] = jnp.zeros((T, LANES), BF16)
    kvb_ref[:, KW : KW + 2 * G] = bias_ref[...]
    pl.semaphore_wait(barrier, 3 + (HI - 1))

    class Piece:
        def __init__(self, view, rows, send, recv, half):
            self.view, self.rows, self.send, self.recv, self.half = view, rows, send, recv, half

        def full(self, j):
            return self.view(j, 0, self.rows)

        def part(self, j, h):
            return self.view(j, h * (self.rows // 2), self.rows // 2)

        def direct(self, z, src=None):
            j = z * LO + lo
            src = self.full(j) if src is None else src
            return [
                remote(src, self.full(j), self.send.at[z * 4 + k], self.recv.at[j], hi * LO + p, c)
                for k, p in enumerate((lo1, lo2))
            ]

        def diag(self, z):
            a, b = z * LO + lo1, z * LO + lo2
            first, last = self.part(a, 0), self.part(b, 1)
            return [
                remote(first, first, self.send.at[z * 4 + 2], self.recv.at[a], hi * LO + lo2, c),
                remote(last, last, self.send.at[z * 4 + 3], self.half.at[z], hi * LO + lo1, c),
            ]

        def arrived(self, ref, sem):
            remote(ref, ref, self.send.at[0], sem, s, other).wait_recv()

        def wait_own(self, z):
            j = z * LO + lo
            self.arrived(self.full(j), self.recv.at[j])

        def wait_direct(self, z):
            for p in (lo1, lo2):
                j = z * LO + p
                self.arrived(self.full(j), self.recv.at[j])

        def wait_diag(self, z):
            j = z * LO + lo3
            self.arrived(self.part(j, 0), self.recv.at[j])
            self.arrived(self.part(j, 1), self.half.at[z])

    kv = Piece(lambda j, r, n: kv_buf.at[pl.ds(j * T + r, n)], T, kv_sp, kv_recv, kv_half)
    up = Piece(lambda j, r, n: up_buf.at[pl.ds(j * R + r, n)], R, up_sp, up_recv, up_half)
    dn = Piece(lambda j, r, n: dn_buf.at[j, pl.ds(r, n)], CH, dn_sp, dn_recv, dn_half)
    up_own = up_ref.at[:, own_cols]
    dn_own = dn_ref.at[pl.ds(hi * CH, CH)]

    def start(copies):
        for copy in copies:
            copy.start()

    def below(dz):
        return (hi - dz + HI) % HI

    def kv_up(hp):
        return remote(kvb_ref, kv.full(s), kv_sz.at[hp], kv_recv.at[s], hp * LO + lo, c)

    def up_far(hp):
        cols = pl.ds(hp * CH, CH)
        return remote(up_ref.at[:, cols], up.full(s), wz_send.at[2 * hp], up_recv.at[s], hp * LO + lo, c)

    def dn_far(hp):
        rows = pl.ds(hp * CH, CH)
        return remote(dn_ref.at[rows], dn.full(s), wz_send.at[2 * hp + 1], dn_recv.at[s], hp * LO + lo, c)

    for hp in range(HI):

        @pl.when(hp > hi)
        def _():
            kv_up(hp).start()

    start(kv.direct(hi, kvb_ref))
    for far in (up_far, dn_far):
        for hp in range(HI - 2, -1, -1):

            @pl.when(hp < hi)
            def _():
                far(hp).start()

    start(up.direct(hi, up_own))
    kv_buf[pl.ds(s * T, T), :] = kvb_ref[...]
    lane = lax.broadcasted_iota(jnp.int32, (T, LANES), 1)
    low = lane < HEAD
    for g in range(G):
        qg = q_ref[:, g * LANES : (g + 1) * LANES].astype(F32) * 0.125
        first = jnp.where(low, qg, 0.0)
        second = jnp.where(low, pltpu.roll(qg, HEAD, 1), 0.0)
        q_buf[g] = jnp.concatenate([first, second], axis=0).astype(BF16)
    row_id = lax.broadcasted_iota(jnp.int32, (PL, PL), 0)
    col_id = lax.broadcasted_iota(jnp.int32, (PL, PL), 1)
    tri_buf[...] = jnp.where(col_id > row_id, 1.0, 0.0).astype(BF16)
    carry[...] = jnp.zeros_like(carry)
    acc[...] = jnp.zeros_like(acc)

    sel_row = lax.broadcasted_iota(jnp.int32, (LANES, LANES), 0) // HEAD
    sel_lane = lax.broadcasted_iota(jnp.int32, (LANES, LANES), 1)
    key_row = lax.broadcasted_iota(jnp.int32, (PL, LANES), 0)
    query_pos = s * T + lax.broadcasted_iota(jnp.int32, (PL, LANES), 1) % T

    def attend(plane):
        rows = pl.ds(plane * PL, PL)
        bias = kv_buf[rows, KW : KW + LANES]
        strict = plane * PL + key_row < query_pos
        for g in range(G):
            pairs = kv_buf[rows, g * LANES : (g + 1) * LANES]
            pick = jnp.where(sel_lane == 2 * g + sel_row, 1.0, 0.0).astype(BF16)
            scores = dot_nt(pairs, q_buf[g]) + dot_nt(bias, pick)
            soft = jnp.maximum(scores, 0.0) + jnp.log(1.0 + jnp.exp(-jnp.abs(scores)))
            log_pass = jnp.where(strict, -soft, 0.0)
            top = log_pass.astype(BF16)
            rest = (log_pass - top.astype(F32)).astype(BF16)
            after = jnp.dot(tri_buf[...], top, preferred_element_type=F32) + jnp.dot(
                tri_buf[...], rest, preferred_element_type=F32
            )
            held = carry[g]
            weights = jnp.where(strict, jnp.exp(scores - soft + after + held), 0.0).astype(BF16)
            acc[g] += dot_tn(weights, pairs)
            carry[g] = held + after[0:1] + log_pass[0:1]

    def column(k):
        @pl.when(k <= hi)
        def _():
            kv.wait_own(hi - k)
            start(kv.direct(hi - k))

    def relay(k):
        @pl.when(k <= hi)
        def _():
            kv.wait_direct(hi - k)
            start(kv.diag(hi - k))

    def look(k):
        @pl.when(k <= hi)
        def _():
            kv.wait_diag(hi - k)
            attend(hi - k)

    def up_column(dz):
        up.wait_own(below(dz))
        start(up.direct(below(dz)))

    def up_relay(dz):
        up.wait_direct(below(dz))
        start(up.diag(below(dz)))

    def dn_column(dz):
        dn.wait_own(below(dz))
        start(dn.direct(below(dz)))

    def dn_relay(dz):
        dn.wait_direct(below(dz))
        start(dn.diag(below(dz)))

    for k in range(1, HI):
        column(k)
        relay(k - 1)
        if k == 1:
            for far in (up_far, dn_far):
                for hp in range(1, HI):

                    @pl.when(hp > hi)
                    def _():
                        far(hp).start()

        if k >= 2:
            look(k - 2)
    relay(HI - 1)
    up_column(1)
    up_relay(0)
    if HI >= 2:
        look(HI - 2)
    for dz in range(2, HI):
        up_column(dz)
    start(dn.direct(hi, dn_own))
    look(HI - 1)
    up_relay(1)

    for load in loads:
        load.wait()
    for g in range(G):
        a0 = pltpu.roll(acc[g, 0:T, :], HEAD, 1)
        a1 = acc[g, T : 2 * T, :]
        att_buf[:, g * LANES : (g + 1) * LANES] = jnp.where(low, a0, a1).astype(BF16)
    att = att_buf[...]
    wide = 512 if D % 512 == 0 else LANES
    for i in range(D // wide):
        cols = slice(i * wide, (i + 1) * wide)
        pj_buf[:, cols] = jnp.dot(att, wo_ref[:, cols], preferred_element_type=F32).astype(BF16)

    pj_copy = remote(pj_buf.at[pl.ds(other * H, H)], pj_in, pj_send, pj_recv, s, other)
    pj_copy.start()
    for dz in range(2, HI):
        up_relay(dz)
    pj_copy.wait()
    mine = pl.ds(c * H, H)
    total = pj_buf[mine, :].astype(F32) + pj_in[...].astype(F32)
    residual = (tok_ref[mine, :].astype(F32) + total).astype(BF16)
    res_buf[...] = residual
    values = residual.astype(F32)
    factor = lax.rsqrt(jnp.mean(values * values, axis=-1, keepdims=True) + EPSILON)

    def n_at(z, core):
        return n_buf.at[pl.ds((core * HI + z) * H, H)]

    n_buf[pl.ds((c * HI + hi) * H, H), :] = (values * factor * gain_ref[...]).astype(BF16)

    def n_out(dz):
        hp = (hi + dz) % HI
        return remote(n_at(hi, c), n_at(hi, c), n_send.at[dz], n_recv.at[c * HI + hi], hp * LO + lo, c)

    def n_pass(dz):
        z = below(dz)
        return remote(n_at(z, c), n_at(z, c), nf_send.at[dz], n_recv.at[c * HI + z], s, other)

    def n_wait(z, core):
        ref = n_at(z, core)
        remote(ref, ref, nf_send.at[0], n_recv.at[core * HI + z], s, other).wait_recv()

    for dz in range(1, HI):
        n_out(dz).start()
    n_pass(0).start()
    for dz in range(1, HI):
        dn_column(dz)
    dn_relay(0)
    for dz in range(1, HI):
        n_wait(below(dz), c)
        n_pass(dz).start()
    for dz in range(HI):
        up.wait_diag(below(dz))
    for dz in range(HI):
        n_wait(below(dz), other)

    step = 256 if CH % 256 == 0 else LANES
    for i in range(CH // step):
        cols = slice(i * step, (i + 1) * step)
        raw = jnp.maximum(jnp.dot(n_buf[...], up_buf[:, cols], preferred_element_type=F32), 0.0)
        hid_buf[:, cols] = (raw * raw).astype(BF16)

    half = HI * H

    def x_out(dz):
        z = below(dz)
        rows = pl.ds(other * half, half)
        return remote(ps_buf.at[z, rows], x_in.at[z], x_send.at[dz], x_recv.at[z], s, other)

    def p_out(dz, far):
        z = below(dz)
        hp = (hi + far) % HI
        return remote(
            xs_buf.at[z, pl.ds(hp * H, H)],
            pr_buf.at[hi, z],
            p_send.at[dz * HI + far],
            p_recv.at[hi * HI + z],
            hp * LO + lo,
            c,
        )

    def p_wait(src, z):
        ref = pr_buf.at[src, z]
        remote(ref, ref, p_send.at[0], p_recv.at[src * HI + z], s, other).wait_recv()

    def spread(dz):
        z = below(dz)
        x_in_ref = x_in.at[z]
        remote(x_in_ref, x_in_ref, x_send.at[0], x_recv.at[z], s, other).wait_recv()
        mixed = ps_buf[z, pl.ds(c * half, half), :].astype(F32) + x_in[z].astype(F32)
        xs_buf[z] = mixed.astype(BF16)
        for far in range(1, HI):
            p_out(dz, far).start()

    for dz in range(HI):
        if dz + 1 < HI:
            dn_relay(dz + 1)
        z = below(dz)
        dn.wait_diag(z)
        for q in range(0, LO, 2):
            pair = jnp.concatenate([dn_buf[z * LO + q], dn_buf[z * LO + q + 1]], axis=1)
            part = jnp.dot(hid_buf[...], pair, preferred_element_type=F32)
            ps_buf[z, :, q * W : (q + 2) * W] = part.astype(BF16)
        x_out(dz).start()
        if dz > 0:
            spread(dz - 1)
    spread(HI - 1)
    CW = LO * W
    for dz in range(HI):
        z = below(dz)
        cols = pl.ds(pl.multiple_of(z * CW, LANES), CW)
        update = xs_buf[z, pl.ds(hi * H, H), :].astype(F32)
        for far in range(1, HI):
            p_wait(below(far), z)
            update = update + pr_buf[below(far), z].astype(F32)
        out_ref[:, cols] = (res_buf[:, cols].astype(F32) + update).astype(BF16)

    for hp in range(HI):

        @pl.when(hp > hi)
        def _():
            kv_up(hp).wait_send()

        @pl.when(hp <= hi)
        def _():
            for copy in kv.direct(hp) + kv.diag(hp):
                copy.wait_send()

        @pl.when(hp != hi)
        def _():
            up_far(hp).wait_send()
            dn_far(hp).wait_send()

        for copy in up.direct(hp) + up.diag(hp) + dn.direct(hp) + dn.diag(hp):
            copy.wait_send()

    for dz in range(HI):
        n_pass(dz).wait_send()
        x_out(dz).wait_send()
        if dz > 0:
            n_out(dz).wait_send()
        for far in range(1, HI):
            p_out(dz, far).wait_send()


def fits(tokens, queries, key_values, stop_bias, up_proj, down_proj):
    sp = lax.axis_size("sp")
    rows, seqs, heads = stop_bias.shape
    hidden = up_proj.shape[1]
    return (
        lax.axis_size("tp") == 2
        and sp % LO == 0
        and sp > LO
        and seqs == 1
        and heads <= LANES
        and queries.shape[2] == heads * HEAD
        and key_values.shape[2] == heads * HEAD
        and 2 * HEAD == LANES
        and 2 * rows == LANES
        and hidden % (sp // LO * LANES) == 0
        and down_proj.shape[1] % LANES == 0
        and up_proj.shape[0] % 16 == 0
        and tokens.shape[2] % LANES == 0
    )


def body(tokens, queries, key_values, stop_bias, out_proj, norm_gain, up_proj, down_proj):
    if not fits(tokens, queries, key_values, stop_bias, up_proj, down_proj):
        return general_body(
            tokens, queries, key_values, stop_bias, out_proj, norm_gain, up_proj, down_proj
        )
    sp = lax.axis_size("sp")
    HI = sp // LO
    T, _, D = tokens.shape
    H = T // 2
    heads = stop_bias.shape[2]
    G = heads // 2
    R, hidden = up_proj.shape
    CH = hidden // HI
    W = down_proj.shape[1]
    KB = G * LANES + LANES
    vmem = pl.BlockSpec(memory_space=pltpu.VMEM)
    hbm = pl.BlockSpec(memory_space=pl.ANY)
    dma = pltpu.SemaphoreType.DMA
    out = pl.pallas_call(
        lambda *refs: layer_kernel(HI, G, *refs),
        out_shape=jax.ShapeDtypeStruct((H, D), BF16),
        in_specs=[vmem, vmem, vmem, vmem, hbm, vmem, hbm, hbm],
        out_specs=vmem,
        scratch_shapes=[
            pltpu.VMEM((T, KB), BF16),
            pltpu.VMEM(out_proj.shape, BF16),
            dma((3,)),
            pltpu.VMEM((sp * T, KB), BF16),
            pltpu.VMEM((sp * R, CH), BF16),
            pltpu.VMEM((sp, CH, W), BF16),
            pltpu.VMEM((G, LANES, LANES), BF16),
            pltpu.VMEM((LO * T, LO * T), BF16),
            pltpu.VMEM((G, 1, LANES), F32),
            pltpu.VMEM((G, LANES, LANES), F32),
            pltpu.VMEM((T, G * LANES), BF16),
            pltpu.VMEM((T, D), BF16),
            pltpu.VMEM((H, D), BF16),
            pltpu.VMEM((H, D), BF16),
            pltpu.VMEM((HI * T, D), BF16),
            pltpu.VMEM((HI * T, CH), BF16),
            pltpu.VMEM((HI, HI * T, LO * W), BF16),
            pltpu.VMEM((HI, HI * H, LO * W), BF16),
            pltpu.VMEM((HI, HI * H, LO * W), BF16),
            pltpu.VMEM((HI, HI, H, LO * W), BF16),
            dma((HI,)),
            dma((HI * 4,)),
            dma((sp,)),
            dma((HI,)),
            dma((HI * 2,)),
            dma((HI * 4,)),
            dma((sp,)),
            dma((HI,)),
            dma((HI * 4,)),
            dma((sp,)),
            dma((HI,)),
            dma,
            dma,
            dma((HI,)),
            dma((HI,)),
            dma((HI * 2,)),
            dma((HI,)),
            dma((HI,)),
            dma((HI * HI,)),
            dma((HI * HI,)),
        ],
        compiler_params=pltpu.CompilerParams(
            collective_id=0, has_side_effects=True, vmem_limit_bytes=56 * 1024 * 1024
        ),
        name="layer",
    )(
        tokens.reshape(T, D),
        queries.reshape(T, queries.shape[2]),
        key_values.reshape(T, key_values.shape[2]),
        stop_bias.reshape(T, heads),
        out_proj,
        norm_gain.reshape(1, D),
        up_proj,
        down_proj,
    )
    return out.reshape(H, 1, D)


def solution(mesh):
    return jax.shard_map(
        body,
        mesh=mesh,
        in_specs=(
            P("sp", None, None),
            P("sp", None, "tp"),
            P("sp", None, "tp"),
            P("sp", None, "tp"),
            P("tp", None),
            P(),
            P("sp", "tp"),
            P("tp", "sp"),
        ),
        out_specs=P(("sp", "tp"), None, None),
        check_vma=False,
    )
```
